32 devices in a mesh: fs: 8 (over z, x), tp: 4 (over y, core).
Axes of the slice: x: 2, y: 2, z: 4, core: 2. Of those that a mesh axis runs over, the one named last changes fastest.
Arguments:
- seq_rows: bfloat16 [6144, 2048], P('fs', 'tp'), may hold values from -6 to 6
- mixer_gain: bfloat16 [2048], P('tp'), may hold values from 0.099609375 to 1.8984375
- query_weight: bfloat16 [2048, 2048], P('fs', 'tp'), may hold values from -0.125 to 0.125
- key_weight: bfloat16 [2048, 2048], P('fs', 'tp'), may hold values from -0.125 to 0.125
- value_weight: bfloat16 [2048, 4096], P('fs', 'tp'), may hold values from -0.125 to 0.125
- decay_logs: float32 [8], P('tp'), may hold values from -0.0333333333 to -0.000390625
- mixer_out_weight: bfloat16 [4096, 2048], P('tp', 'fs'), may hold values from -0.125 to 0.125
- channel_gain: bfloat16 [2048], P('tp'), may hold values from 0.099609375 to 1.8984375
- value_up_weight: bfloat16 [2048, 5632], P('fs', 'tp'), may hold values from -0.125 to 0.125
- gate_up_weight: bfloat16 [2048, 5632], P('fs', 'tp'), may hold values from -0.125 to 0.125
- conv_taps: bfloat16 [3, 5632], P(None, 'tp'), may hold values from -3 to 3
- conv_bias: bfloat16 [5632], P('tp'), may hold values from -3 to 3
- down_weight: bfloat16 [5632, 2048], P('tp', 'fs'), may hold values from -0.109375 to 0.109375
Outputs:
- layer_out: bfloat16 [6144, 2048], P('fs', 'tp')
The draws below stay inside these ranges and needn't reach their ends.
All inputs are finite; a program needn't handle non-finite values.
Results may differ from the reference program's by a relative error of at most 0.02.
Values may be sent and summed in bfloat16 or wider, within the bound.
A program may use at most 128 MiB of HBM per device.

```python
import jax
import jax.numpy as jnp
from jax import lax

D = 2048
HEADS = 8
DK = 256
DV = 512
FF = 5632
KW = 3
BLOCK = 128
SEQ_LEN = 768
TOKENS = 6144
N_TP = 4


def draw_decay_logs(key, part):
    pick_key = jax.random.fold_in(key, 11)
    fast_key = jax.random.fold_in(key, 12)
    slow_key = jax.random.fold_in(key, 13)
    order = jax.random.permutation(pick_key, HEADS)
    quick = order < HEADS // 2
    fast = -1.0 / jax.random.uniform(fast_key, (HEADS,), jnp.float32, 30.0, 100.0)
    slow = -jax.random.uniform(slow_key, (HEADS,), jnp.float32, 0.3, 2.0) / SEQ_LEN
    return jnp.where(quick, fast, slow).astype(jnp.float32)


def strengthened(array, own_key, source, target, blocks, factor):
    def block_of(dim):
        return (jnp.arange(array.shape[dim]) // (array.shape[dim] // blocks)).reshape((-1,) + (1,) * (array.ndim - 1 - dim))

    one_side = jax.random.permutation(own_key, blocks)[block_of(target)]
    far = (block_of(target) + blocks // 2) % blocks
    return jnp.where((block_of(source) == one_side) | (block_of(source) == far), factor * array, array)


def levels(key, shape, split, least, high):
    level, own = 1.0, jax.random.fold_in(key, 6)
    for dim, parts in split:
        heights = jnp.exp(jax.random.uniform(jax.random.fold_in(own, dim), (parts,), jnp.float32, least / len(split), high / len(split)))
        level = level * jnp.repeat(heights, shape[dim] // parts).reshape([-1 if axis == dim else 1 for axis in range(len(shape))])
    return level


def scatter_about(rng, shape, scale, most, pieces=(), kind=jnp.bfloat16):
    gain = levels(rng, shape, pieces, -0.22, 0.18) if pieces else 1.0
    values = jax.random.normal(rng, shape, jnp.float32) * scale * gain
    return jnp.minimum(jnp.maximum(values, -most), most).astype(kind)


def noise_with(own_key, dims, scale, limit, split, heavy, kind=jnp.bfloat16):
    drawn = scale * jax.random.normal(own_key, dims, jnp.float32)
    if split:
        drawn = drawn * levels(own_key, dims, split, -0.22, 0.18)
    return jnp.clip(strengthened(drawn, jax.random.fold_in(own_key, 3), *heavy), -limit, limit).astype(kind)


def setup_inputs(seed: int = 0) -> dict:
    keys = jax.random.split(jax.random.key(seed), 14)
    seq_rows = scatter_about(keys[0], (TOKENS, D), 1.0, 6.0, ((0, 8), (1, 4)))
    mixer_gain = jnp.clip(1.0 + 0.18 * jax.random.normal(keys[1], (D,), jnp.float32), 0.099609375, 1.8984375).astype(jnp.bfloat16)
    query_weight = scatter_about(keys[2], (D, HEADS * DK), D ** -0.5, 0.125, ((0, 8), (1, 4)))
    key_weight = scatter_about(keys[3], (D, HEADS * DK), D ** -0.5, 0.125, ((0, 8), (1, 4)))
    value_weight = scatter_about(keys[4], (D, HEADS * DV), D ** -0.5, 0.125, ((0, 8), (1, 4)))
    decay_logs = draw_decay_logs(jax.random.fold_in(keys[13], 71), 0)
    mixer_out_weight = noise_with(keys[6], (HEADS * DV, D), (HEADS * DV) ** -0.5, 0.125, ((0, 4), (1, 8)), (0, 1, 8, 2.0))
    channel_gain = jnp.clip(1.0 + 0.18 * jax.random.normal(keys[7], (D,), jnp.float32), 0.099609375, 1.8984375).astype(jnp.bfloat16)
    value_up_weight = scatter_about(keys[8], (D, FF), D ** -0.5, 0.125, ((0, 8), (1, 4)))
    gate_up_weight = scatter_about(keys[9], (D, FF), D ** -0.5, 0.125, ((0, 8), (1, 4)))
    conv_taps = scatter_about(keys[10], (KW, FF), 0.6, 3.0, ((1, 4),))
    conv_bias = scatter_about(keys[11], (FF,), 0.5, 3.0, ((0, 4),))
    down_weight = noise_with(keys[12], (FF, D), FF ** -0.5, 0.109375, ((0, 4), (1, 8)), (0, 1, 8, 2.0))
    return dict(seq_rows=seq_rows, mixer_gain=mixer_gain, query_weight=query_weight, key_weight=key_weight, value_weight=value_weight, decay_logs=decay_logs, mixer_out_weight=mixer_out_weight, channel_gain=channel_gain, value_up_weight=value_up_weight, gate_up_weight=gate_up_weight, conv_taps=conv_taps, conv_bias=conv_bias, down_weight=down_weight)


EPS = 1e-06
ROPE_BASE = 10000.0
HIGH_PRECISION = lax.Precision.HIGHEST

def rotate_heads(tensor, cosine, sine):
    half = tensor.shape[-1] // 2
    first = tensor[..., :half]
    second = tensor[..., half:]
    return jnp.concatenate([first * cosine - second * sine, first * sine + second * cosine], axis=-1)

def retention_blocks(query, key, value, decay_logs):
    length, heads = (query.shape[0], query.shape[1])
    count = length // BLOCK
    offsets = jnp.arange(BLOCK, dtype=jnp.float32)
    spread = offsets[:, None] - offsets[None, :]
    within_block = jnp.where(spread[None] >= 0.0, jnp.exp(decay_logs[:, None, None] * jnp.maximum(spread, 0.0)[None]), 0.0)
    carried = jnp.exp(decay_logs[:, None] * (offsets + 1.0))
    state_decay_factor = jnp.exp(decay_logs[:, None] * (BLOCK - 1.0 - offsets))
    block_decay_factor = jnp.exp(decay_logs * BLOCK)

    def blocks(tensor):
        return tensor.reshape(count, BLOCK, heads, tensor.shape[-1]).transpose(0, 2, 1, 3)

    def advance(recurrent_state, triple):
        query_block, key_block, value_block = triple
        attention_scores = jnp.einsum('ucf,uxf->ucx', query_block, key_block, precision=HIGH_PRECISION) * within_block
        result = jnp.einsum('hnm,hmv->hnv', attention_scores, value_block, precision=HIGH_PRECISION)
        result = result + jnp.einsum('hnd,hdv->hnv', query_block, recurrent_state, precision=HIGH_PRECISION) * carried[:, :, None]
        recurrent_state = block_decay_factor[:, None, None] * recurrent_state + jnp.einsum('ieb,iez->ibz', key_block * state_decay_factor[:, :, None], value_block, precision=HIGH_PRECISION)
        return (recurrent_state, result)
    start = jnp.zeros((heads, query.shape[-1], value.shape[-1]), jnp.float32)
    _, result = lax.scan(advance, start, (blocks(query), blocks(key), blocks(value)))
    return result.transpose(0, 2, 1, 3).reshape(length, heads, value.shape[-1])

def grouped_sum(left, right, groups):
    width = left.shape[1] // groups

    def add_group(index, total):
        begin = (index * width).astype(jnp.int32)
        term = jnp.dot(lax.dynamic_slice_in_dim(left, begin, width, 1), lax.dynamic_slice_in_dim(right, begin, width, 0), preferred_element_type=jnp.float32)
        rounded = lax.optimization_barrier(term.astype(jnp.bfloat16))
        return total + rounded.astype(jnp.float32)
    start = jnp.zeros((left.shape[0], right.shape[1]), jnp.float32)
    return lax.fori_loop(jnp.int32(0), jnp.int32(groups), add_group, start)

def one_sequence(rows, mixer_gain, query_weight, key_weight, value_weight, decay_logs, mixer_out_weight, channel_gain, value_up_weight, gate_up_weight, conv_taps, conv_bias, down_weight):
    length = rows.shape[0]
    rows_f = rows.astype(jnp.float32)
    scale_one = lax.rsqrt(lax.optimization_barrier(jnp.mean(rows_f * rows_f, axis=-1, keepdims=True)) + EPS)
    scaled_one = (rows_f * mixer_gain.astype(jnp.float32)).astype(jnp.bfloat16)
    query = (jnp.dot(scaled_one, query_weight, preferred_element_type=jnp.float32) * scale_one).astype(jnp.bfloat16)
    key = (jnp.dot(scaled_one, key_weight, preferred_element_type=jnp.float32) * scale_one).astype(jnp.bfloat16)
    value = (jnp.dot(scaled_one, value_weight, preferred_element_type=jnp.float32) * scale_one).astype(jnp.bfloat16)
    half = DK // 2
    freqs = jnp.power(ROPE_BASE, -jnp.arange(half, dtype=jnp.float32) * 2.0 / DK)
    angles = jnp.arange(length, dtype=jnp.float32)[:, None] * freqs[None, :]
    cosine = jnp.cos(angles)[:, None, :]
    sine = jnp.sin(angles)[:, None, :]
    turned_q = rotate_heads(query.astype(jnp.float32).reshape(length, HEADS, DK), cosine, sine)
    turned_k = rotate_heads(key.astype(jnp.float32).reshape(length, HEADS, DK), cosine, sine) * DK ** (-0.5)
    ret = retention_blocks(turned_q, turned_k, value.astype(jnp.float32).reshape(length, HEADS, DV), decay_logs)
    centred = ret - lax.optimization_barrier(jnp.mean(ret, axis=-1, keepdims=True))
    normed = (centred * lax.rsqrt(lax.optimization_barrier(jnp.mean(centred * centred, axis=-1, keepdims=True)) + EPS)).reshape(length, HEADS * DV).astype(jnp.bfloat16)
    mixed = grouped_sum(normed, mixer_out_weight, N_TP)
    middle = (rows_f + mixed).astype(jnp.bfloat16)
    middle_f = middle.astype(jnp.float32)
    scale_two = lax.rsqrt(lax.optimization_barrier(jnp.mean(middle_f * middle_f, axis=-1, keepdims=True)) + EPS)
    scaled_two = (middle_f * channel_gain.astype(jnp.float32)).astype(jnp.bfloat16)
    up_val = (jnp.dot(scaled_two, value_up_weight, preferred_element_type=jnp.float32) * scale_two).astype(jnp.bfloat16)
    up_gate = (jnp.dot(scaled_two, gate_up_weight, preferred_element_type=jnp.float32) * scale_two).astype(jnp.bfloat16)
    padded = jnp.concatenate([jnp.zeros((KW - 1, FF), jnp.float32), up_gate.astype(jnp.float32)], axis=0)
    conv = jnp.zeros((length, FF), jnp.float32) + conv_bias.astype(jnp.float32)[None, :]
    for tap in range(KW):
        conv = conv + conv_taps[tap].astype(jnp.float32)[None, :] * padded[tap:tap + length]
    hidden = (jax.nn.silu(conv) * up_val.astype(jnp.float32)).astype(jnp.bfloat16)
    channel = grouped_sum(hidden, down_weight, N_TP)
    return (middle_f + channel).astype(jnp.bfloat16)

def reference(seq_rows, mixer_gain, query_weight, key_weight, value_weight, decay_logs, mixer_out_weight, channel_gain, value_up_weight, gate_up_weight, conv_taps, conv_bias, down_weight):
    sequences = seq_rows.reshape(TOKENS // SEQ_LEN, SEQ_LEN, D)

    def run(rows):
        return one_sequence(rows, mixer_gain, query_weight, key_weight, value_weight, decay_logs, mixer_out_weight, channel_gain, value_up_weight, gate_up_weight, conv_taps, conv_bias, down_weight)
    return lax.map(run, sequences).reshape(TOKENS, D)
```

```python
import jax
import jax.numpy as jnp
from jax import lax
from jax.sharding import PartitionSpec as P

DK = 256
DV = 512
KW = 3


EPS = 1e-06
ROPE_BASE = 10000.0


def rotate_heads(tensor, cosine, sine):
    half = tensor.shape[-1] // 2
    first = tensor[..., :half]
    second = tensor[..., half:]
    return jnp.concatenate(
        [first * cosine - second * sine, first * sine + second * cosine], axis=-1
    )


def retention(query, key, value, decay_logs):
    length = query.shape[0]
    offsets = jnp.arange(length, dtype=jnp.float32)
    spread = offsets[:, None] - offsets[None, :]
    out = []
    for head in range(query.shape[1]):
        decay = jnp.where(
            spread >= 0.0, jnp.exp(decay_logs[head] * jnp.maximum(spread, 0.0)), 0.0
        )
        scores = lax.dot_general(
            query[:, head],
            key[:, head],
            (((1,), (1,)), ((), ())),
            preferred_element_type=jnp.float32,
        )
        scores = (scores * decay).astype(jnp.bfloat16)
        out.append(jnp.dot(scores, value[:, head], preferred_element_type=jnp.float32))
    return out


def ring_order(count):
    return list(range(0, count, 2)) + list(range(count - 1, 0, -2))


class Stream:
    def __init__(self, block, count):
        order = ring_order(count)
        self.count = count
        self.ahead = [(order[i], order[(i + 1) % count]) for i in range(count)]
        self.back = [(to, frm) for frm, to in self.ahead]
        self.held = {0: block}
        self.moving = (block, block)
        self.step = 0

    def hop(self, after):
        if after is not None:
            self.moving, after.held = lax.optimization_barrier((self.moving, after.held))
            if after.step < after.count // 2:
                after.moving = (after.held[after.count - after.step], after.held[after.step])
        self.step += 1
        one, two = self.moving
        last = self.step == self.count // 2
        if last:
            half = one.shape[0] // 2
            one, two = one[:half], two[half:]
        one = lax.ppermute(one, "fs", self.ahead)
        two = lax.ppermute(two, "fs", self.back)
        if last:
            self.held[self.step] = jnp.concatenate([one, two], axis=0)
        else:
            self.held[self.count - self.step] = one
            self.held[self.step] = two
            self.moving = (one, two)

    def blocks(self):
        return [self.held[d] for d in range(self.count)]


def pick(tensor, index, width):
    return lax.dynamic_slice_in_dim(tensor, index * width, width, 1)


def gather_tp(part):
    size = lax.axis_size("tp")
    me = lax.axis_index("tp")
    bit = size // 2
    whole = [part]
    found = part
    bits = []
    while bit > 1:
        bits.append(bit)
        bit //= 2
    bits = bits[::-1] + [1]
    for bit in bits:
        other = lax.ppermute(found, "tp", [(t, t ^ bit) for t in range(size)])
        found = jnp.concatenate([found, other], axis=1)
    width = part.shape[1]
    code = [0]
    for bit in bits:
        code = code + [c ^ bit for c in code]
    place = {c: i for i, c in enumerate(code)}

    def column_block(owner):
        flip = jnp.bitwise_xor(owner, me)
        table = jnp.array([place[c] for c in range(size)], jnp.int32)
        return lax.dynamic_index_in_dim(table, flip, keepdims=False)

    return found, column_block


def scatter_tp(terms):
    size = lax.axis_size("tp")
    me = lax.axis_index("tp")
    width = terms.shape[1] // size
    current, left, bit = terms, size, 1
    while left > 1:
        mine = jnp.bitwise_and(me // bit, 1)
        keep = jnp.concatenate([pick(current, 2 * k + mine, width) for k in range(left // 2)], axis=1)
        send = jnp.concatenate(
            [pick(current, 2 * k + 1 - mine, width) for k in range(left // 2)], axis=1
        )
        got = lax.ppermute(send, "tp", [(t, t ^ bit) for t in range(size)])
        current = keep.astype(jnp.float32) + got.astype(jnp.float32)
        left //= 2
        bit *= 2
        if left > 1:
            current = current.astype(jnp.bfloat16)
    return current


def normalise(whole_rows, gain_row):
    rows_f = whole_rows.astype(jnp.float32)
    factor = lax.rsqrt(jnp.mean(rows_f * rows_f, axis=-1, keepdims=True) + EPS)
    scaled = (rows_f * gain_row.astype(jnp.float32)[None, :]).astype(jnp.bfloat16)
    return (factor, scaled)


def on_device(
    seq_rows,
    mixer_gain,
    query_weight,
    key_weight,
    value_weight,
    decay_logs,
    mixer_out_weight,
    channel_gain,
    value_up_weight,
    gate_up_weight,
    conv_taps,
    conv_bias,
    down_weight,
):
    length = seq_rows.shape[0]
    heads_here = query_weight.shape[1] // DK
    count = lax.axis_size("fs")
    tp_size = lax.axis_size("tp")
    order = jnp.array(ring_order(count), jnp.int32)
    places = [0] * count
    for place, owner in enumerate(ring_order(count)):
        places[owner] = place
    spot = lax.dynamic_index_in_dim(
        jnp.array(places, jnp.int32), lax.axis_index("fs"), keepdims=False
    )
    ids = [
        lax.dynamic_index_in_dim(order, lax.rem(spot + d, count), keepdims=False)
        for d in range(count)
    ]

    gate_half = gate_up_weight.shape[1] // 2
    streams = [
        Stream(jnp.concatenate([query_weight, key_weight], axis=1), count),
        Stream(value_weight, count),
        Stream(mixer_out_weight, count),
        Stream(value_up_weight, count),
        Stream(gate_up_weight[:, :gate_half], count),
        Stream(gate_up_weight[:, gate_half:], count),
        Stream(down_weight[: down_weight.shape[0] // 2], count),
        Stream(down_weight[down_weight.shape[0] // 2 :], count),
    ]

    extra = jnp.concatenate(
        [mixer_gain[None], channel_gain[None], jnp.zeros((14, mixer_gain.shape[0]), jnp.bfloat16)],
        axis=0,
    )
    found, block_of = gather_tp(jnp.concatenate([seq_rows, extra], axis=0))

    for pair in range(0, len(streams), 2):
        for step in range(count // 2):
            for which in (0, 1):
                stream = streams[pair + which]
                before = streams[pair - 2 + which] if step == 0 and pair else None
                stream.hop(before)

    chunk = query_weight.shape[0]
    per_owner = seq_rows.shape[1] // chunk

    def in_ring_order(found):
        return jnp.concatenate(
            [
                pick(found, block_of(j // per_owner) * per_owner + lax.rem(j, per_owner), chunk)
                for j in ids
            ],
            axis=1,
        )

    ordered = in_ring_order(found)
    factor_one, scaled_one = normalise(ordered[:length], ordered[length])
    gain_two = ordered[length + 1]
    weight_qk = jnp.concatenate(streams[0].blocks(), axis=0)
    weight_v = jnp.concatenate(streams[1].blocks(), axis=0)
    sum_qk = jnp.dot(scaled_one, weight_qk, preferred_element_type=jnp.float32)
    sum_v = jnp.dot(scaled_one, weight_v, preferred_element_type=jnp.float32)
    wide = query_weight.shape[1]
    query = (sum_qk[:, :wide] * factor_one).astype(jnp.bfloat16)
    key = (sum_qk[:, wide:] * factor_one).astype(jnp.bfloat16)
    value = (sum_v * factor_one).astype(jnp.bfloat16)
    half = DK // 2
    freqs = jnp.power(ROPE_BASE, -jnp.arange(half, dtype=jnp.float32) * 2.0 / DK)
    angles = jnp.arange(length, dtype=jnp.float32)[:, None] * freqs[None, :]
    cosine = jnp.cos(angles)
    sine = jnp.sin(angles)
    normed = []
    for head in range(heads_here):
        q = query[:, head * DK : (head + 1) * DK].astype(jnp.float32)
        k = key[:, head * DK : (head + 1) * DK].astype(jnp.float32)
        v = value[:, head * DV : (head + 1) * DV]
        turned_q = rotate_heads(q, cosine, sine).astype(jnp.bfloat16)
        turned_k = (rotate_heads(k, cosine, sine) * DK ** (-0.5)).astype(jnp.bfloat16)
        ret = retention(turned_q[:, None], turned_k[:, None], v[:, None], decay_logs[head : head + 1])[0]
        centred = ret - jnp.mean(ret, axis=-1, keepdims=True)
        normed.append(
            (
                centred * lax.rsqrt(jnp.mean(centred * centred, axis=-1, keepdims=True) + EPS)
            ).astype(jnp.bfloat16)
        )
    normed = jnp.concatenate(normed, axis=1)

    def in_place(pieces, width):
        whole = jnp.zeros((length, width * count), jnp.bfloat16)
        for j, piece in zip(ids, pieces):
            whole = lax.dynamic_update_slice(whole, piece, (0, j * width))
        return whole

    columns = mixer_out_weight.shape[1]
    mixed_terms = in_place(
        [
            jnp.dot(normed, block, preferred_element_type=jnp.float32).astype(jnp.bfloat16)
            for block in streams[2].blocks()
        ],
        columns,
    )
    mixed = scatter_tp(mixed_terms)
    middle = (seq_rows.astype(jnp.float32) + mixed).astype(jnp.bfloat16)
    found, block_of = gather_tp(middle)
    factor_two, scaled_two = normalise(in_ring_order(found), gain_two)
    weight_val = jnp.concatenate(streams[3].blocks(), axis=0)
    up_val = (
        jnp.dot(scaled_two, weight_val, preferred_element_type=jnp.float32) * factor_two
    ).astype(jnp.bfloat16)
    hidden = []
    for part in (0, 1):
        cut = slice(part * gate_half, (part + 1) * gate_half)
        weight_gate = jnp.concatenate(streams[4 + part].blocks(), axis=0)
        sum_gate = jnp.dot(scaled_two, weight_gate, preferred_element_type=jnp.float32)
        up_gate = (sum_gate * factor_two).astype(jnp.bfloat16)
        padded = jnp.concatenate(
            [jnp.zeros((KW - 1, gate_half), jnp.bfloat16), up_gate], axis=0
        )
        conv = conv_bias[cut].astype(jnp.float32)[None, :]
        for tap in range(KW):
            conv = conv + conv_taps[tap, cut].astype(jnp.float32)[None, :] * padded[
                tap : tap + length
            ].astype(jnp.float32)
        hidden.append((jax.nn.silu(conv) * up_val[:, cut].astype(jnp.float32)).astype(jnp.bfloat16))
    hidden = jnp.concatenate(hidden, axis=1)
    channel_terms = in_place(
        [
            jnp.dot(
                hidden, jnp.concatenate([one, two], axis=0), preferred_element_type=jnp.float32
            ).astype(jnp.bfloat16)
            for one, two in zip(streams[6].blocks(), streams[7].blocks())
        ],
        columns,
    )
    channel = scatter_tp(channel_terms)
    return (middle.astype(jnp.float32) + channel).astype(jnp.bfloat16)


def solution(mesh):
    placed = (
        P("fs", "tp"),
        P("tp"),
        P("fs", "tp"),
        P("fs", "tp"),
        P("fs", "tp"),
        P("tp"),
        P("tp", "fs"),
        P("tp"),
        P("fs", "tp"),
        P("fs", "tp"),
        P(None, "tp"),
        P("tp"),
        P("tp", "fs"),
    )
    return jax.shard_map(
        on_device, mesh=mesh, in_specs=placed, out_specs=P("fs", "tp"), check_vma=False
    )
```

```python
import jax
import jax.numpy as jnp
from jax import lax
from jax.sharding import PartitionSpec as P

DK = 256
DV = 512
KW = 3


EPS = 1e-06
ROPE_BASE = 10000.0


def rotate_heads(tensor, cosine, sine):
    half = tensor.shape[-1] // 2
    first = tensor[..., :half]
    second = tensor[..., half:]
    return jnp.concatenate(
        [first * cosine - second * sine, first * sine + second * cosine], axis=-1
    )


def retention(query, key, value, decay_logs):
    length = query[0].shape[0]
    offsets = jnp.arange(length, dtype=jnp.float32)
    spread = offsets[:, None] - offsets[None, :]
    out = []
    decays = jnp.where(
        (spread >= 0.0)[None],
        jnp.exp(decay_logs[:, None, None] * jnp.maximum(spread, 0.0)[None]),
        0.0,
    )
    for head in range(len(query)):
        scores = lax.dot_general(
            query[head],
            key[head],
            (((1,), (1,)), ((), ())),
            preferred_element_type=jnp.float32,
        )
        scores = (scores * decays[head]).astype(jnp.bfloat16)
        out.append(jnp.dot(scores, value[head], preferred_element_type=jnp.float32))
    return out


def ring_order(count):
    return list(range(0, count, 2)) + list(range(count - 1, 0, -2))


def ring_place(owner, count):
    return jnp.where(lax.rem(owner, 2) == 0, owner // 2, count - (owner + 1) // 2)


def ring_owner(place, count):
    return jnp.where(place < count // 2, 2 * place, 2 * (count - place) - 1)


class Stream:
    def __init__(self, block, count):
        order = ring_order(count)
        self.count = count
        self.ahead = [(order[i], order[(i + 1) % count]) for i in range(count)]
        self.back = [(to, frm) for frm, to in self.ahead]
        self.held = {0: block}
        self.moving = (block, block)
        self.step = 0

    def hop(self, after):
        if after is not None:
            self.moving, after.held = lax.optimization_barrier((self.moving, after.held))
            if after.step < after.count // 2:
                after.moving = (after.held[after.count - after.step], after.held[after.step])
        self.step += 1
        one, two = self.moving
        last = self.step == self.count // 2
        if last:
            half = one.shape[0] // 2
            one, two = one[:half], two[half:]
        one = lax.ppermute(one, "fs", self.ahead)
        two = lax.ppermute(two, "fs", self.back)
        if last:
            self.held[self.step] = jnp.concatenate([one, two], axis=0)
        else:
            self.held[self.count - self.step] = one
            self.held[self.step] = two
            self.moving = (one, two)

    def blocks(self):
        return [self.held[d] for d in range(self.count)]


def pick(tensor, index, width):
    return lax.dynamic_slice_in_dim(tensor, index * width, width, 1)


def gather_tp(part):
    size = lax.axis_size("tp")
    me = lax.axis_index("tp")
    bit = size // 2
    whole = [part]
    found = part
    bits = []
    while bit > 1:
        bits.append(bit)
        bit //= 2
    bits = bits[::-1] + [1]
    for bit in bits:
        other = lax.ppermute(found, "tp", [(t, t ^ bit) for t in range(size)])
        found = jnp.concatenate([found, other], axis=1)
    width = part.shape[1]
    code = [0]
    for bit in bits:
        code = code + [c ^ bit for c in code]
    place = {c: i for i, c in enumerate(code)}

    def column_block(owner):
        flip = jnp.bitwise_xor(owner, me)
        return sum(jnp.bitwise_and(flip // bit, 1) * place[bit] for bit in bits)

    return found, column_block


def scatter_tp(terms):
    size = lax.axis_size("tp")
    me = lax.axis_index("tp")
    width = terms.shape[1] // size
    current, left, bit = terms, size, 1
    while left > 1:
        mine = jnp.bitwise_and(me // bit, 1)
        keep = jnp.concatenate([pick(current, 2 * k + mine, width) for k in range(left // 2)], axis=1)
        send = jnp.concatenate(
            [pick(current, 2 * k + 1 - mine, width) for k in range(left // 2)], axis=1
        )
        got = lax.ppermute(send, "tp", [(t, t ^ bit) for t in range(size)])
        current = keep.astype(jnp.float32) + got.astype(jnp.float32)
        left //= 2
        bit *= 2
        if left > 1:
            current = current.astype(jnp.bfloat16)
    return current


def normalise(whole_rows, gain_row):
    rows_f = whole_rows.astype(jnp.float32)
    factor = lax.rsqrt(jnp.mean(rows_f * rows_f, axis=-1, keepdims=True) + EPS)
    scaled = (rows_f * gain_row.astype(jnp.float32)[None, :]).astype(jnp.bfloat16)
    return (factor, scaled)


def on_device(
    seq_rows,
    mixer_gain,
    query_weight,
    key_weight,
    value_weight,
    decay_logs,
    mixer_out_weight,
    channel_gain,
    value_up_weight,
    gate_up_weight,
    conv_taps,
    conv_bias,
    down_weight,
):
    length = seq_rows.shape[0]
    heads_here = query_weight.shape[1] // DK
    count = lax.axis_size("fs")
    tp_size = lax.axis_size("tp")
    spot = ring_place(lax.axis_index("fs"), count)
    ids = [ring_owner(lax.rem(spot + d, count), count) for d in range(count)]

    gate_half = gate_up_weight.shape[1] // 2
    streams = [
        Stream(jnp.concatenate([query_weight, key_weight], axis=1), count),
        Stream(value_weight, count),
        Stream(mixer_out_weight, count),
        Stream(value_up_weight, count),
        Stream(gate_up_weight[:, :gate_half], count),
        Stream(gate_up_weight[:, gate_half:], count),
        Stream(down_weight[: down_weight.shape[0] // 2], count),
        Stream(down_weight[down_weight.shape[0] // 2 :], count),
    ]

    extra = jnp.concatenate(
        [mixer_gain[None], channel_gain[None], jnp.zeros((14, mixer_gain.shape[0]), jnp.bfloat16)],
        axis=0,
    )
    found, block_of = gather_tp(jnp.concatenate([seq_rows, extra], axis=0))

    hops = count // 2
    late = streams[-2:]
    for pair in range(0, len(streams), 2):
        for step in range(hops):
            for which in (0, 1):
                stream = streams[pair + which]
                if pair and step == 0:
                    continue
                if stream not in late or step < hops - 2:
                    stream.hop(None)
                if pair + 2 < len(streams) and step == hops - 2:
                    streams[pair + 2 + which].hop(stream)

    chunk = query_weight.shape[0]
    per_owner = seq_rows.shape[1] // chunk

    def in_ring_order(found):
        return jnp.concatenate(
            [
                pick(found, block_of(j // per_owner) * per_owner + lax.rem(j, per_owner), chunk)
                for j in ids
            ],
            axis=1,
        )

    ordered = in_ring_order(found)
    factor_one, scaled_one = normalise(ordered[:length], ordered[length])
    gain_two = ordered[length + 1]
    weight_qk = jnp.concatenate(streams[0].blocks(), axis=0)
    weight_v = jnp.concatenate(streams[1].blocks(), axis=0)
    sum_qk = jnp.dot(scaled_one, weight_qk, preferred_element_type=jnp.float32)
    sum_v = jnp.dot(scaled_one, weight_v, preferred_element_type=jnp.float32)
    wide = query_weight.shape[1]
    query = (sum_qk[:, :wide] * factor_one).astype(jnp.bfloat16)
    key = (sum_qk[:, wide:] * factor_one).astype(jnp.bfloat16)
    value = (sum_v * factor_one).astype(jnp.bfloat16)
    half = DK // 2
    freqs = jnp.power(ROPE_BASE, -jnp.arange(half, dtype=jnp.float32) * 2.0 / DK)
    angles = jnp.arange(length, dtype=jnp.float32)[:, None] * freqs[None, :]
    cosine = jnp.cos(angles)
    sine = jnp.sin(angles)
    turned_q, turned_k, values = [], [], []
    for head in range(heads_here):
        q = query[:, head * DK : (head + 1) * DK].astype(jnp.float32)
        k = key[:, head * DK : (head + 1) * DK].astype(jnp.float32)
        turned_q.append(rotate_heads(q, cosine, sine).astype(jnp.bfloat16))
        turned_k.append((rotate_heads(k, cosine, sine) * DK ** (-0.5)).astype(jnp.bfloat16))
        values.append(value[:, head * DV : (head + 1) * DV])
    normed = []
    for ret in retention(turned_q, turned_k, values, decay_logs):
        centred = ret - jnp.mean(ret, axis=-1, keepdims=True)
        normed.append(
            (
                centred * lax.rsqrt(jnp.mean(centred * centred, axis=-1, keepdims=True) + EPS)
            ).astype(jnp.bfloat16)
        )
    normed = jnp.concatenate(normed, axis=1)

    def in_place(pieces, width):
        whole = jnp.zeros((length, width * count), jnp.bfloat16)
        for j, piece in zip(ids, pieces):
            whole = lax.dynamic_update_slice(whole, piece, (0, j * width))
        return whole

    columns = mixer_out_weight.shape[1]
    mixed_terms = in_place(
        [
            jnp.dot(normed, block, preferred_element_type=jnp.float32).astype(jnp.bfloat16)
            for block in streams[2].blocks()
        ],
        columns,
    )
    mixed = scatter_tp(mixed_terms)
    middle = (seq_rows.astype(jnp.float32) + mixed).astype(jnp.bfloat16)
    found, block_of = gather_tp(middle)
    factor_two, scaled_two = normalise(in_ring_order(found), gain_two)
    weight_val = jnp.concatenate(streams[3].blocks(), axis=0)
    up_val = (
        jnp.dot(scaled_two, weight_val, preferred_element_type=jnp.float32) * factor_two
    ).astype(jnp.bfloat16)
    hidden = []
    for part in (0, 1):
        cut = slice(part * gate_half, (part + 1) * gate_half)
        weight_gate = jnp.concatenate(streams[4 + part].blocks(), axis=0)
        sum_gate = jnp.dot(scaled_two, weight_gate, preferred_element_type=jnp.float32)
        up_gate = (sum_gate * factor_two).astype(jnp.bfloat16)
        padded = jnp.concatenate(
            [jnp.zeros((KW - 1, gate_half), jnp.bfloat16), up_gate], axis=0
        )
        conv = conv_bias[cut].astype(jnp.float32)[None, :]
        for tap in range(KW):
            conv = conv + conv_taps[tap, cut].astype(jnp.float32)[None, :] * padded[
                tap : tap + length
            ].astype(jnp.float32)
        hidden.append((jax.nn.silu(conv) * up_val[:, cut].astype(jnp.float32)).astype(jnp.bfloat16))
    hidden = jnp.concatenate(hidden, axis=1)
    one, two = late
    one.moving, two.moving, hidden = lax.optimization_barrier((one.moving, two.moving, hidden))
    one.hop(None)
    two.hop(None)

    def term(d):
        block = jnp.concatenate([one.held[d], two.held[d]], axis=0)
        return jnp.dot(hidden, block, preferred_element_type=jnp.float32).astype(jnp.bfloat16)

    early = {d: term(d) for d in range(count) if min(d, count - d) <= hops - 2}
    one.moving, two.moving, early = lax.optimization_barrier((one.moving, two.moving, early))
    one.hop(None)
    two.hop(None)
    channel_terms = in_place([early[d] if d in early else term(d) for d in range(count)], columns)
    channel = scatter_tp(channel_terms)
    return (middle.astype(jnp.float32) + channel).astype(jnp.bfloat16)


def solution(mesh):
    placed = (
        P("fs", "tp"),
        P("tp"),
        P("fs", "tp"),
        P("fs", "tp"),
        P("fs", "tp"),
        P("tp"),
        P("tp", "fs"),
        P("tp"),
        P("fs", "tp"),
        P("fs", "tp"),
        P(None, "tp"),
        P("tp"),
        P("tp", "fs"),
    )
    return jax.shard_map(
        on_device, mesh=mesh, in_specs=placed, out_specs=P("fs", "tp"), check_vma=False
    )
```
